32 devices in a mesh: sp: 8 (over z, y), tp: 4 (over x, core).
Axes of the slice: x: 2, y: 2, z: 4, core: 2. Of those that a mesh axis runs over, the one named last changes fastest.
Arguments:
- frames: bfloat16 [4, 1024, 1024], P('tp', 'sp'), may hold values from -22 to 22
- norm_gain: float32 [1024], replicated, may hold values from 0.5 to 1.5
- conv_value_w: bfloat16 [1024, 512], P(None, 'tp'), may hold values from -0.1875 to 0.1875
- conv_gate_w: bfloat16 [1024, 512], P(None, 'tp'), may hold values from -0.1875 to 0.1875
- conv_taps: bfloat16 [31, 512], P(None, 'tp'), may hold values from -1 to 1
- conv_bias: float32 [512], P('tp'), may hold values from -1.2 to 1.2
- channel_gain: float32 [512], P('tp'), may hold values from 0.5 to 1.5
- channel_shift: float32 [512], P('tp'), may hold values from -1.2 to 1.2
- query_w: bfloat16 [1024, 1024], P(None, 'tp'), may hold values from -0.1875 to 0.1875
- forget_w: bfloat16 [1024, 1024], P(None, 'tp'), may hold values from -0.1875 to 0.1875
- input_w: bfloat16 [1024, 1024], P(None, 'tp'), may hold values from -0.1875 to 0.1875
- gate_w: bfloat16 [1024, 1024], P(None, 'tp'), may hold values from -0.1875 to 0.1875
- memory_rate: float32 [1024], P('tp'), may hold values from 0.5 to 32
- head_gain: float32 [1024], P('tp'), may hold values from 0.5 to 1.5
- conv_out_w: bfloat16 [512, 1024], P('tp'), may hold values from -0.1875 to 0.1875
- rec_out_w: bfloat16 [1024, 1024], P('tp'), may hold values from -0.125 to 0.125
Outputs:
- mixed: bfloat16 [4, 1024, 1024], P('tp', 'sp')
The draws below stay inside these ranges and needn't reach their ends.
All inputs are finite; a program needn't handle non-finite values.
Results may differ from the reference program's by a relative error of at most 0.015.
The reference program's roundings to bfloat16 on the way (of `normed`, `gated_conv`, `conv_out`, `scores`, `carried_low` and `rec_out`) count: a program that leaves them out, or rounds other values in their place, can miss the bound.
Values may be sent and summed in bfloat16 or wider, within the bound.
No kernel may reach another device: no remote copies, remote signals or barrier semaphores. Data moves between devices by JAX's collectives and lax.ppermute only.
A program may use at most 64 MiB of HBM per device.

```python
import math
import jax
import jax.numpy as jnp
from jax import lax

D = 1024
D_CONV = 512
CONV_WIDTH = 31
HEADS = 8
HEAD = 128
D_HG = 1024
POS_DEV = 128
SEQS = 4
SEQ_LEN = 1024
N_SP = 8


def draw_frames(key, part):
    noise_key = jax.random.fold_in(key, 11)
    direction_key = jax.random.fold_in(key, 12)
    level_key = jax.random.fold_in(key, 13)
    block_count = SEQ_LEN // POS_DEV
    noise = jnp.clip(jax.random.normal(noise_key, (SEQS, SEQ_LEN, D), jnp.float32), -6.0, 6.0)
    direction = jnp.clip(jax.random.normal(direction_key, (D,), jnp.float32), -4.0, 4.0)
    levels = jax.random.uniform(level_key, (SEQS, block_count, 1, 1), jnp.float32, -4.0, 4.0)
    spread_levels = jnp.broadcast_to(levels, (SEQS, block_count, POS_DEV, 1)).reshape(SEQS, SEQ_LEN, 1)
    return (noise + spread_levels * direction).astype(jnp.bfloat16)


def shard_levels(stream_key, extent, pieces, low, largest):
    def one(dim, blocks):
        draws = jax.random.uniform(jax.random.fold_in(jax.random.fold_in(stream_key, 6), dim), (blocks,), jnp.float32, low / len(pieces), largest / len(pieces))
        return jnp.repeat(jnp.exp(draws), extent[dim] // blocks).reshape((-1,) + (1,) * (len(extent) - dim - 1))

    gain = one(*pieces[0])
    for cut in pieces[1:]:
        gain = gain * one(*cut)
    return gain


def bell_draw(key, dims, deviation, most, shards=(), held_as=jnp.bfloat16):
    values = deviation * jax.random.normal(key, dims, jnp.float32)
    if shards:
        values = values * shard_levels(key, dims, shards, -0.22, 0.18)
    return jnp.clip(values, -most, most).astype(held_as)


def setup_inputs(seed: int = 0) -> dict:
    arg_keys = jax.random.split(jax.random.key(seed), 17)
    return {
        "frames": draw_frames(jax.random.fold_in(arg_keys[16], 71), 0),
        "norm_gain": jnp.clip(1.0 + 0.1 * jax.random.normal(arg_keys[1], (D,), jnp.float32), 0.5, 1.5),
        "conv_value_w": bell_draw(arg_keys[2], (D, D_CONV), D ** -0.5, 0.1875, ((1, 4),)),
        "conv_gate_w": bell_draw(arg_keys[3], (D, D_CONV), D ** -0.5, 0.1875, ((1, 4),)),
        "conv_taps": bell_draw(arg_keys[4], (CONV_WIDTH, D_CONV), CONV_WIDTH ** -0.5, 1.0, ((1, 4),)),
        "conv_bias": bell_draw(arg_keys[5], (D_CONV,), 0.2, 1.2, ((0, 4),), jnp.float32),
        "channel_gain": jnp.clip(1.0 + 0.1 * jax.random.normal(arg_keys[6], (D_CONV,), jnp.float32), 0.5, 1.5),
        "channel_shift": bell_draw(arg_keys[7], (D_CONV,), 0.2, 1.2, ((0, 4),), jnp.float32),
        "query_w": bell_draw(arg_keys[8], (D, D_HG), D ** -0.5, 0.1875, ((1, 4),)),
        "forget_w": bell_draw(arg_keys[9], (D, D_HG), D ** -0.5, 0.1875, ((1, 4),)),
        "input_w": bell_draw(arg_keys[10], (D, D_HG), D ** -0.5, 0.1875, ((1, 4),)),
        "gate_w": bell_draw(arg_keys[11], (D, D_HG), D ** -0.5, 0.1875, ((1, 4),)),
        "memory_rate": jnp.clip(jnp.exp(math.log(32.0) - 4.158883 * jax.random.uniform(arg_keys[12], (D_HG,), jnp.float32) ** shard_levels(arg_keys[12], (D_HG,), ((0, 4),), -0.2, 0.2)), 0.5, 32.0),
        "head_gain": jnp.clip(1.0 + 0.1 * jax.random.normal(arg_keys[13], (D_HG,), jnp.float32), 0.5, 1.5),
        "conv_out_w": bell_draw(arg_keys[14], (D_CONV, D), (2 * D_CONV) ** -0.5, 0.1875, ((0, 4),)),
        "rec_out_w": bell_draw(arg_keys[15], (D_HG, D), (2 * D_HG) ** -0.5, 0.125, ((0, 4),)),
    }


EPS = 1e-06

def reference(frames, norm_gain, conv_value_w, conv_gate_w, conv_taps, conv_bias, channel_gain, channel_shift, query_w, forget_w, input_w, gate_w, memory_rate, head_gain, conv_out_w, rec_out_w):
    values = frames.astype(jnp.float32)
    normed = (values * lax.rsqrt(lax.optimization_barrier(jnp.mean(values * values, axis=-1, keepdims=True)) + EPS) * norm_gain).astype(jnp.bfloat16)
    flat_rows = normed.reshape(SEQS * SEQ_LEN, D)

    def project(weight):
        product = jnp.dot(flat_rows, weight, preferred_element_type=jnp.float32)
        return product.astype(jnp.bfloat16).reshape(SEQS, SEQ_LEN, weight.shape[1])
    conv_value = project(conv_value_w)
    conv_gate = project(conv_gate_w)
    queries = project(query_w)
    forget_raw = project(forget_w)
    inputs = project(input_w)
    out_gate = project(gate_w)
    gated_conv = (conv_value.astype(jnp.float32) * jax.nn.sigmoid(conv_gate.astype(jnp.float32))).astype(jnp.bfloat16)
    filtered = lax.conv_general_dilated(gated_conv, conv_taps[:, None, :], window_strides=(1,), padding=[(CONV_WIDTH - 1, 0)], dimension_numbers=('NWC', 'WIO', 'NWC'), feature_group_count=D_CONV, preferred_element_type=jnp.float32) + conv_bias
    row_mean = lax.optimization_barrier(jnp.mean(filtered, axis=-1, keepdims=True))
    row_var = lax.optimization_barrier(jnp.mean(filtered * filtered, axis=-1, keepdims=True)) - row_mean * row_mean
    scaled = (filtered - row_mean) * lax.rsqrt(row_var + EPS) * channel_gain + channel_shift
    conv_out = jax.nn.silu(scaled).astype(jnp.bfloat16)
    head_shape = (SEQS, SEQ_LEN, HEADS, HEAD)
    rate_rows = (memory_rate / SEQ_LEN).reshape(HEADS, HEAD)
    in_gate = rate_rows * jax.nn.sigmoid(-forget_raw.astype(jnp.float32)).reshape(head_shape)
    log_forget = jnp.log1p(-in_gate)
    query_rows = queries.astype(jnp.float32).reshape(head_shape)
    value_rows = inputs.reshape(head_shape).astype(jnp.float32)

    def to_blocks(array):
        return array.reshape(SEQS, N_SP, POS_DEV, HEADS, HEAD).transpose(1, 0, 2, 3, 4)
    causal = jnp.tril(jnp.ones((POS_DEV, POS_DEV), dtype=bool))
    highest = lax.Precision.HIGHEST

    def advance(carry_state, block_inputs):
        block_query, block_gate, block_forget, block_value = block_inputs
        cumulative = jnp.cumsum(block_forget, axis=1)
        final_sum = cumulative[:, -1]
        grown = (block_query * jnp.exp(cumulative)).astype(jnp.bfloat16).astype(jnp.float32)
        shrunk = (block_gate * jnp.exp(-cumulative)).astype(jnp.bfloat16).astype(jnp.float32)
        weighted = (block_gate * jnp.exp(final_sum[:, None] - cumulative)).astype(jnp.bfloat16).astype(jnp.float32)
        scores = jnp.einsum('sthk,suhk->shtu', grown, shrunk, precision=highest)
        scores = jnp.where(causal, scores, 0.0).astype(jnp.bfloat16).astype(jnp.float32)
        carried_low = carry_state.astype(jnp.bfloat16).astype(jnp.float32)
        block_out = jnp.einsum('shtu,suhv->sthv', scores, block_value, precision=highest)
        block_out = block_out + jnp.einsum('sthk,shkv->sthv', grown, carried_low, precision=highest)
        new_state = jnp.exp(final_sum)[..., None] * carry_state + jnp.einsum('suhk,suhv->shkv', weighted, block_value, precision=highest)
        return (new_state, block_out)
    start_state = jnp.zeros((SEQS, HEADS, HEAD, HEAD), jnp.float32)
    blocks = (to_blocks(query_rows), to_blocks(in_gate), to_blocks(log_forget), to_blocks(value_rows))
    final_state, block_outs = lax.scan(advance, start_state, blocks)
    rec_raw = block_outs.transpose(1, 0, 2, 3, 4).reshape(head_shape)
    rec_norm = rec_raw * lax.rsqrt(lax.optimization_barrier(jnp.mean(rec_raw * rec_raw, axis=-1, keepdims=True)) + EPS) * head_gain.reshape(HEADS, HEAD)
    rec_out = (rec_norm.reshape(SEQS, SEQ_LEN, D_HG) * jax.nn.silu(out_gate.astype(jnp.float32))).astype(jnp.bfloat16)
    conv_part = jnp.dot(conv_out.reshape(SEQS * SEQ_LEN, D_CONV), conv_out_w, preferred_element_type=jnp.float32)
    rec_part = jnp.dot(rec_out.reshape(SEQS * SEQ_LEN, D_HG), rec_out_w, preferred_element_type=jnp.float32)
    return (conv_part + rec_part).astype(jnp.bfloat16).reshape(SEQS, SEQ_LEN, D)
```

```python
import functools
import jax
import jax.numpy as jnp
from jax import lax
from jax.experimental import pallas as pl
from jax.experimental.pallas import tpu as pltpu
from jax.sharding import PartitionSpec as P

HEAD = 128
EPS = 1e-06
EDGE = 32
TAIL = 16
BF16 = jnp.bfloat16
F32 = jnp.float32
AXES = ("sp", "tp")
VMEM_LIMIT = 24 * 1024 * 1024


def route(value, groups, chips, target):
    pairs = []
    for group in range(groups):
        for half in range(2):
            for chip in range(chips):
                for core in range(2):
                    aim = target(group, half, chip, core)
                    if aim is not None:
                        g, h, x, c = aim
                        source = (group * 2 + half) * chips * 2 + chip * 2 + core
                        pairs.append((source, (g * 2 + h) * chips * 2 + x * 2 + c))
    return lax.ppermute(value, AXES, pairs)


def call(body, outs, args, scratch=(), flops=0, size=0):
    spaces = [
        pl.BlockSpec(memory_space=pltpu.SMEM if arg.dtype == jnp.int32 else pltpu.VMEM)
        for arg in args
    ]
    single = not isinstance(outs, (list, tuple))
    shapes = [outs] if single else list(outs)
    result = pl.pallas_call(
        body,
        out_shape=shapes,
        in_specs=spaces,
        out_specs=[pl.BlockSpec(memory_space=pltpu.VMEM)] * len(shapes),
        scratch_shapes=list(scratch),
        compiler_params=pltpu.CompilerParams(vmem_limit_bytes=VMEM_LIMIT),
        cost_estimate=pl.CostEstimate(flops=flops, bytes_accessed=size, transcendentals=0),
    )(*args)
    return result[0] if single else result


def dot(left, right, dims=((1,), (0,)), precision=None):
    return lax.dot_general(
        left, right, (dims, ((), ())), preferred_element_type=F32, precision=precision
    )


def sigmoid(value):
    return 1.0 / (1.0 + jnp.exp(-value))


def begin_kernel(chips, *refs):
    core = refs[0][0]
    pieces = refs[1 : 1 + 2 * chips]
    gain, value_w, gate_w, forget_w, input_w, rate = refs[1 + 2 * chips : 7 + 2 * chips]
    normed_o, gated_o, edge_o, cum_o, in_gate_o, inputs_o, first_o, decay_o, send_o = refs[
        7 + 2 * chips :
    ]
    rows = pieces[0].shape[0]
    heads = rate.shape[1] // HEAD
    lower = lax.broadcasted_iota(jnp.int32, (rows, rows), 1) <= lax.broadcasted_iota(
        jnp.int32, (rows, rows), 0
    )
    lower = lower.astype(F32)
    for k in range(chips):
        mine, other = pieces[2 * k][...], pieces[2 * k + 1][...]
        for half in range(2):
            block = jnp.where(core == half, mine, other).astype(F32)
            scale = lax.rsqrt(jnp.mean(block * block, axis=-1, keepdims=True) + EPS)
            normed_o[k, pl.ds(half * rows, rows), :] = (block * scale * gain[...]).astype(BF16)
        normed = normed_o[k]
        forget_raw = dot(normed, forget_w[...]).astype(BF16).astype(F32)
        inputs = dot(normed, input_w[...]).astype(BF16)
        inputs_o[k] = inputs
        in_gate = rate[...] * sigmoid(-forget_raw)
        in_gate_o[k] = in_gate
        log_forget = jnp.log1p(-in_gate)
        states, lasts = [], []
        for half in range(2):
            part = slice(half * rows, (half + 1) * rows)
            cumulative = dot(lower, log_forget[part], precision=lax.Precision.HIGHEST)
            cum_o[k, pl.ds(half * rows, rows), :] = cumulative
            last = cumulative[rows - 1 : rows]
            weighted = (in_gate[part] * jnp.exp(last - cumulative)).astype(BF16)
            lasts.append(last)
            states.append(
                [
                    dot(
                        inputs[part, h * HEAD : (h + 1) * HEAD],
                        weighted[:, h * HEAD : (h + 1) * HEAD],
                        ((0,), (0,)),
                    )
                    for h in range(heads)
                ]
            )
        decays = [jnp.exp(last) for last in lasts]
        decay_o[k] = jnp.broadcast_to(decays[0], (8, decays[0].shape[1]))
        whole = jnp.exp(lasts[0] + lasts[1])
        high = whole.astype(BF16).astype(F32)
        for h in range(heads):
            cols = slice(h * HEAD, (h + 1) * HEAD)
            first_o[k, h] = states[0][h]
            send_o[k, h, pl.ds(0, HEAD), :] = (
                decays[1][:, cols] * states[0][h] + states[1][h]
            ).astype(BF16)
            spot = lax.broadcasted_iota(jnp.int32, (TAIL, HEAD), 0)
            tail = jnp.where(spot == 0, high[:, cols], (whole - high)[:, cols])
            send_o[k, h, pl.ds(HEAD, TAIL), :] = tail.astype(BF16)
        conv_value = dot(normed, value_w[...]).astype(BF16).astype(F32)
        conv_gate = dot(normed, gate_w[...]).astype(BF16).astype(F32)
        gated = (conv_value * sigmoid(conv_gate)).astype(BF16)
        gated_o[k] = gated
        edge_o[k] = gated[2 * rows - EDGE :]


def middle_kernel(chips, normed, cum, in_gate, inputs, query_w, out_gate_w, *outs):
    grown_o, local_o, gate_o = outs
    rows = normed.shape[1] // 2
    heads = query_w.shape[1] // HEAD
    seen = lax.broadcasted_iota(jnp.int32, (rows, rows), 1) <= lax.broadcasted_iota(
        jnp.int32, (rows, rows), 0
    )
    for k in range(chips):
        queries = dot(normed[k], query_w[...]).astype(BF16).astype(F32)
        gate_o[k] = dot(normed[k], out_gate_w[...]).astype(BF16)
        growth = jnp.exp(cum[k])
        grown = (queries * growth).astype(BF16)
        shrunk = (in_gate[k] * jnp.exp(-cum[k])).astype(BF16)
        grown_o[k] = grown
        for half in range(2):
            part = slice(half * rows, (half + 1) * rows)
            for h in range(heads):
                cols = slice(h * HEAD, (h + 1) * HEAD)
                scores = dot(grown[part, cols], shrunk[part, cols], ((1,), (1,)))
                scores = jnp.where(seen, scores, 0.0).astype(BF16)
                local_o[k, pl.ds(half * rows, rows), pl.ds(h * HEAD, HEAD)] = dot(
                    scores, inputs[k, pl.ds(half * rows, rows), pl.ds(h * HEAD, HEAD)]
                )


def conv_kernel(chips, core, gated, edge, taps, bias, gain, shift, *refs):
    outs, extended = refs[:-1], refs[-1]
    rows = gated.shape[1] // 2
    width = taps.shape[0]
    for k in range(chips):
        extended[pl.ds(0, EDGE), :] = edge[k].astype(F32)
        extended[pl.ds(EDGE, 2 * rows), :] = gated[k].astype(F32)
        for half in range(2):
            total = jnp.broadcast_to(bias[...], (rows, bias.shape[1]))
            for j in range(width):
                start = half * rows + EDGE - (width - 1) + j
                total = total + taps[pl.ds(j, 1), :].astype(F32) * extended[pl.ds(start, rows), :]
            for e in range(2):
                @pl.when((core[0] ^ e) == half)
                def _():
                    outs[2 * k + e][pl.ds(0, rows), :] = total
        spot = lax.broadcasted_iota(jnp.int32, (8, bias.shape[1]), 0)
        for e in range(2):
            outs[2 * k + e][pl.ds(rows, 8), :] = jnp.where(spot == 0, gain[...], shift[...])


def finish_kernel(chips, core, *refs):
    arrived = refs[: -6 - 2 * chips]
    first, decay, grown, local, out_gate, gain = refs[-6 - 2 * chips : -2 * chips]
    outs = refs[-2 * chips :]
    rows = grown.shape[1] // 2
    heads = gain.shape[1] // HEAD
    for k in range(chips):
        for h in range(heads):
            cols = slice(h * HEAD, (h + 1) * HEAD)
            state, span = None, None
            for ref in arrived:
                part = ref[k, h, pl.ds(0, HEAD), :].astype(F32)
                ends = ref[k, h, pl.ds(HEAD, TAIL), :].astype(F32)
                ends = ends[0:1] + ends[1:2]
                state = part if state is None else state + span * part
                span = ends if span is None else span * ends
            later = decay[k, 0:1, cols] * state + first[k, h]
            for e in range(2):
                half = core[0] ^ e
                low = jnp.where(half == 0, state, later).astype(BF16)
                part = pl.ds(pl.multiple_of(half * rows, rows), rows)
                raw = local[k, part, cols] + dot(grown[k, part, cols], low, ((1,), (1,)))
                scale = lax.rsqrt(jnp.mean(raw * raw, axis=-1, keepdims=True) + EPS)
                gate = out_gate[k, part, cols].astype(F32)
                outs[2 * k + e][:, cols] = (
                    raw * scale * gain[:, cols] * (gate * sigmoid(gate))
                ).astype(BF16)


def sorted_pair(swap, first, second):
    return jnp.where(swap, second, first), jnp.where(swap, first, second)


def conv_out_kernel(chips, where, *refs):
    parts, weights, out = refs[: 2 * chips], refs[2 * chips : 4 * chips], refs[4 * chips]
    rows = parts[0].shape[0] - 8
    channels = 2 * chips * parts[0].shape[1]
    values = [part[pl.ds(0, rows), :] for part in parts]
    total = sum(jnp.sum(value, axis=-1, keepdims=True) for value in values)
    square = sum(jnp.sum(value * value, axis=-1, keepdims=True) for value in values)
    mean = total / channels
    scale = lax.rsqrt(square / channels - mean * mean + EPS)
    result = []
    for part, value in zip(parts, values):
        tail = part[pl.ds(rows, 8), :]
        scaled = (value - mean) * scale * tail[0:1] + tail[1:2]
        result.append(scaled * sigmoid(scaled))
    swap = where[0] != where[1]
    total = None
    for k in range(chips):
        near, far = sorted_pair(swap, result[2 * k], result[2 * k + 1])
        term = dot(near.astype(BF16), weights[2 * k][...]) + dot(
            far.astype(BF16), weights[2 * k + 1][...]
        )
        total = term if total is None else total + term
    out[...] = total


def rec_out_kernel(chips, where, conv_part, *refs):
    parts, weights, out = refs[: 2 * chips], refs[2 * chips : 4 * chips], refs[4 * chips]
    swap = where[0] != where[1]
    total = conv_part[...]
    for k in range(chips):
        near, far = sorted_pair(swap, parts[2 * k][...], parts[2 * k + 1][...])
        total = total + dot(near, weights[2 * k][...]) + dot(far, weights[2 * k + 1][...])
    out[...] = total.astype(BF16)


def local(
    frames,
    norm_gain,
    conv_value_w,
    conv_gate_w,
    conv_taps,
    conv_bias,
    channel_gain,
    channel_shift,
    query_w,
    forget_w,
    input_w,
    gate_w,
    memory_rate,
    head_gain,
    conv_out_w,
    rec_out_w,
):
    assert frames.shape[0] == 1
    groups, chips = lax.axis_size("sp") // 2, lax.axis_size("tp") // 2
    rows, width = frames.shape[1:]
    conv_local, rec_local = conv_value_w.shape[1], query_w.shape[1]
    heads = rec_local // HEAD
    seq_total = rows * lax.axis_size("sp")
    half = (lax.axis_index("sp") % 2).astype(jnp.int32)
    core = (lax.axis_index("tp") % 2).astype(jnp.int32)
    core_s = core.reshape(1)
    where_s = jnp.stack([half, core])
    send = functools.partial(route, groups=groups, chips=chips)
    shape = jax.ShapeDtypeStruct

    def partner(value):
        return send(value, target=lambda g, h, x, c: (g, h, x, 1 - c))

    def shifted(value, k):
        return send(value, target=lambda g, h, x, c: (g, h, (x + k) % chips, c))

    pieces = []
    flat = frames[0]
    for k in range(chips):
        mine = send(flat, target=lambda g, h, x, c: (g, c, (x + k) % chips, h))
        pieces += [mine, partner(mine)]

    conv_weights, rec_weights = [], []
    for k in range(chips):
        for weight, kept in ((conv_out_w, conv_weights), (rec_out_w, rec_weights)):
            near = weight if k == 0 else shifted(weight, k)
            kept += [near, partner(near)]

    row = lambda vector: vector.reshape(1, -1)
    span = 2 * rows
    normed, gated, edge, cum, in_gate, inputs, first, decay, packet = call(
        functools.partial(begin_kernel, chips),
        [
            shape((chips, span, width), BF16),
            shape((chips, span, conv_local), BF16),
            shape((chips, EDGE, conv_local), BF16),
            shape((chips, span, rec_local), F32),
            shape((chips, span, rec_local), F32),
            shape((chips, span, rec_local), BF16),
            shape((chips, heads, HEAD, HEAD), F32),
            shape((chips, 8, rec_local), F32),
            shape((chips, heads, HEAD + TAIL, HEAD), BF16),
        ],
        [core_s, *pieces, row(norm_gain), conv_value_w, conv_gate_w, forget_w, input_w,
         row(memory_rate / seq_total)],
        flops=2 * chips * span * width * (2 * conv_local + 2 * rec_local),
        size=1 << 21,
    )

    def later(value, steps):
        return send(
            value,
            target=lambda g, h, x, c: (g + steps, h, x, c) if g + steps < groups else None,
        )

    before = later(edge, 1)
    arrived = [later(packet, steps) for steps in range(1, groups)]

    grown, local_out, out_gate = call(
        functools.partial(middle_kernel, chips),
        [
            shape((chips, span, rec_local), BF16),
            shape((chips, span, rec_local), F32),
            shape((chips, span, rec_local), BF16),
        ],
        [normed, cum, in_gate, inputs, query_w, gate_w],
        flops=2 * chips * span * width * 2 * rec_local,
        size=1 << 21,
    )
    filtered = call(
        functools.partial(conv_kernel, chips),
        [shape((rows + 8, conv_local), F32)] * (2 * chips),
        [core_s, gated, before, conv_taps, row(conv_bias), row(channel_gain), row(channel_shift)],
        scratch=[pltpu.VMEM((span + EDGE, conv_local), F32)],
        flops=1 << 28,
        size=1 << 20,
    )

    def home(parts):
        result = []
        for k in range(chips):
            for e in range(2):
                part = parts[2 * ((chips - k) % chips) + e]
                result.append(
                    send(part, target=lambda g, h, x, c: (g, c ^ e, (x + k) % chips, h))
                )
        return result

    conv_part = call(
        functools.partial(conv_out_kernel, chips),
        shape((rows, width), F32),
        [where_s, *home(filtered), *conv_weights],
        flops=2 * rows * width * 2 * chips * conv_local,
        size=1 << 20,
    )
    rec_out = call(
        functools.partial(finish_kernel, chips),
        [shape((rows, rec_local), BF16)] * (2 * chips),
        [core_s, *arrived, first, decay, grown, local_out, out_gate, row(head_gain)],
        flops=1 << 28,
        size=1 << 21,
    )
    mixed = call(
        functools.partial(rec_out_kernel, chips),
        shape((rows, width), BF16),
        [where_s, conv_part, *home(rec_out), *rec_weights],
        flops=2 * rows * width * 2 * chips * rec_local,
        size=1 << 21,
    )
    return mixed[None]


def solution(mesh):
    placed = (
        P("tp", "sp", None),
        P(),
        P(None, "tp"),
        P(None, "tp"),
        P(None, "tp"),
        P("tp"),
        P("tp"),
        P("tp"),
        P(None, "tp"),
        P(None, "tp"),
        P(None, "tp"),
        P(None, "tp"),
        P("tp"),
        P("tp"),
        P("tp", None),
        P("tp", None),
    )
    return jax.shard_map(
        local, mesh=mesh, in_specs=placed, out_specs=P("tp", "sp", None), check_vma=False
    )
```
